32 devices in a mesh: sp: 4 (over y, x), tp: 8 (over z, core).
Axes of the slice: x: 2, y: 2, z: 4, core: 2. Of those that a mesh axis runs over, the one named last changes fastest.
Arguments:
- tokens: bfloat16 [8, 512, 4096], P('tp', 'sp'), may hold values from -6 to 6
- latent_down_matrix: bfloat16 [4096, 512], P('tp'), may hold values from -0.09375 to 0.09375
- rope_weight: bfloat16 [4096, 64], P('tp'), may hold values from -0.09375 to 0.09375
- latent_norm_scale: float32 [512], replicated, may hold values from 0.1 to 1.9
- key_up_matrix: bfloat16 [512, 32, 128], P(None, 'tp'), may hold values from -0.25 to 0.25
- value_up_matrix: bfloat16 [512, 32, 128], P(None, 'tp'), may hold values from -0.25 to 0.25
- query: bfloat16 [8, 32, 192], P('sp', 'tp'), may hold values from -126 to 126
Outputs:
- plain_key_cache: bfloat16 [8, 512, 32, 128], P('sp', None, 'tp')
- head_value_cache: bfloat16 [8, 512, 32, 128], P('sp', None, 'tp')
- rotated_key_cache: bfloat16 [8, 512, 64], P('sp')
- first_read: bfloat16 [8, 32, 128], P('sp', 'tp')
The draws below stay inside these ranges and needn't reach their ends.
All inputs are finite; a program needn't handle non-finite values.
Results may differ from the reference program's by a relative error of at most 0.035.
Values may be sent and summed in bfloat16 or wider, within the bound.
A program may use at most 64 MiB of HBM per device.

```python
import jax
import jax.numpy as jnp
from jax import lax

MODEL_WIDTH = 4096
LATENT_WIDTH = 512
ROPE = 64
PLAIN_KEY_WIDTH = 128
VALUE_WIDTH = 128
ATTENTION_HEADS = 32
SEQUENCE_COUNT = 8
SEQUENCE_LENGTH = 512


def draw_query(key, part):
    base = jnp.clip(jax.random.normal(jax.random.fold_in(key, 11), (SEQUENCE_COUNT, ATTENTION_HEADS, PLAIN_KEY_WIDTH + ROPE), jnp.float32), -3.5, 3.5) * 3.0
    return base.astype(jnp.bfloat16)


def block_scale(key, dims, split, least, top_value):
    level = 1.0
    for dim, parts in split:
        heights = jax.random.uniform(jax.random.fold_in(jax.random.fold_in(key, 6), dim), (parts,), jnp.float32, least / len(split), top_value / len(split))
        level = level * jnp.repeat(jnp.exp(heights), dims[dim] // parts).reshape((-1,) + (1,) * (len(dims) - 1 - dim))
    return level


def gaussian(rng, shape, scale, most, cuts=(), kind=jnp.bfloat16):
    factor_of = block_scale(rng, shape, cuts, -0.22, 0.18) if cuts else 1.0
    array = jax.random.normal(rng, shape, jnp.float32) * scale * factor_of
    return jnp.minimum(jnp.maximum(array, -most), most).astype(kind)


def setup_inputs(seed: int = 0) -> dict:
    key_list = jax.random.split(jax.random.key(seed), 8)
    return {
        "tokens": gaussian(key_list[0], (SEQUENCE_COUNT, SEQUENCE_LENGTH, MODEL_WIDTH), 1.0, 6.0, ((0, 8), (1, 4))),
        "latent_down_matrix": gaussian(key_list[1], (MODEL_WIDTH, LATENT_WIDTH), MODEL_WIDTH ** -0.5, 0.09375, ((0, 8),)),
        "rope_weight": gaussian(key_list[2], (MODEL_WIDTH, ROPE), MODEL_WIDTH ** -0.5, 0.09375, ((0, 8),)),
        "latent_norm_scale": jnp.clip(1.0 + 0.18 * jax.random.normal(key_list[3], (LATENT_WIDTH,), jnp.float32), 0.1, 1.9),
        "key_up_matrix": gaussian(key_list[4], (LATENT_WIDTH, ATTENTION_HEADS, PLAIN_KEY_WIDTH), LATENT_WIDTH ** -0.5, 0.25, ((1, 8),)),
        "value_up_matrix": gaussian(key_list[5], (LATENT_WIDTH, ATTENTION_HEADS, VALUE_WIDTH), LATENT_WIDTH ** -0.5, 0.25, ((1, 8),)),
        "query": draw_query(jax.random.fold_in(key_list[7], 71), 0),
    }


def rotate(part, positions):
    half = part.shape[-1] // 2
    freqs = 1.0 / 10000.0 ** (jnp.arange(half, dtype=jnp.float32) * 2.0 / part.shape[-1])
    angles = positions.astype(jnp.float32)[:, None] * freqs
    cosine = jnp.cos(angles)
    sine = jnp.sin(angles)
    first = part[..., :half]
    second = part[..., half:]
    return jnp.concatenate([first * cosine - second * sine, second * cosine + first * sine], axis=-1)

def reference(tokens, latent_down_matrix, rope_weight, latent_norm_scale, key_up_matrix, value_up_matrix, query):
    flat = tokens.reshape(SEQUENCE_COUNT * SEQUENCE_LENGTH, MODEL_WIDTH)
    latent = jnp.dot(flat, latent_down_matrix, preferred_element_type=jnp.float32)
    scaled = latent * lax.rsqrt(lax.optimization_barrier(jnp.mean(latent * latent, axis=-1, keepdims=True)) + 1e-06)
    latent_normalized = (scaled * latent_norm_scale.astype(jnp.float32)).astype(jnp.bfloat16)
    rope = jnp.dot(flat, rope_weight, preferred_element_type=jnp.float32).reshape(SEQUENCE_COUNT, SEQUENCE_LENGTH, ROPE)
    positions = jnp.arange(SEQUENCE_LENGTH, dtype=jnp.int32)
    rotated_key_cache = rotate(rope, positions).astype(jnp.bfloat16)
    plain_key_cache = jnp.dot(latent_normalized, key_up_matrix.reshape(LATENT_WIDTH, ATTENTION_HEADS * PLAIN_KEY_WIDTH), preferred_element_type=jnp.float32).astype(jnp.bfloat16).reshape(SEQUENCE_COUNT, SEQUENCE_LENGTH, ATTENTION_HEADS, PLAIN_KEY_WIDTH)
    head_value_cache = jnp.dot(latent_normalized, value_up_matrix.reshape(LATENT_WIDTH, ATTENTION_HEADS * VALUE_WIDTH), preferred_element_type=jnp.float32).astype(jnp.bfloat16).reshape(SEQUENCE_COUNT, SEQUENCE_LENGTH, ATTENTION_HEADS, VALUE_WIDTH)
    query_float = query.astype(jnp.float32)
    query_plain = query[..., :PLAIN_KEY_WIDTH]
    rotated_query = rotate(query_float[..., PLAIN_KEY_WIDTH:], jnp.full((1,), SEQUENCE_LENGTH, jnp.int32)).astype(jnp.bfloat16)
    factor = 1.0 / (PLAIN_KEY_WIDTH + ROPE) ** 0.5

    def attend(items):
        plain, turned, keys, values, rotary = items
        scores = jnp.einsum('hd,lhd->hl', plain.astype(jnp.float32), keys.astype(jnp.float32))
        scores = scores + jnp.einsum('hd,ld->hl', turned.astype(jnp.float32), rotary.astype(jnp.float32))
        scores = scores * factor
        weights = jnp.exp(scores - lax.optimization_barrier(jnp.max(scores, axis=-1, keepdims=True)))
        total = lax.optimization_barrier(jnp.sum(weights, axis=-1, keepdims=True))
        rounded = weights.astype(jnp.bfloat16)
        mixed = jnp.einsum('hl,lhd->hd', rounded.astype(jnp.float32), values.astype(jnp.float32))
        return (mixed / total).astype(jnp.bfloat16)
    first_read = lax.map(attend, (query_plain, rotated_query, plain_key_cache, head_value_cache, rotated_key_cache))
    return (plain_key_cache, head_value_cache, rotated_key_cache, first_read)
```

```python
import functools

import numpy as np
import jax
import jax.numpy as jnp
from jax import lax
from jax.sharding import PartitionSpec as P
from jax.experimental import pallas as pl
from jax.experimental.pallas import tpu as pltpu

CORES = 2
PARTS = 4
LAG = 4
VMEM_BYTES = 32 * 1024 * 1024
BF16 = jnp.bfloat16
F32 = jnp.float32


def turn_tables(positions, width):
    half = width // 2
    freqs = (1.0 / np.float32(10000.0) ** (np.arange(half, dtype=np.float32) * np.float32(2.0) / np.float32(width))).astype(np.float32)
    angles = positions.astype(np.float32)[:, None] * freqs
    cosine = np.cos(angles).astype(np.float32)
    sine = np.sin(angles).astype(np.float32)
    return np.concatenate([cosine, cosine], -1), np.concatenate([-sine, sine], -1)


def turn(part, cosine, sine):
    half = part.shape[-1] // 2
    swapped = jnp.concatenate([part[:, half:], part[:, :half]], axis=-1)
    return part * cosine + swapped * sine


def move_kernel(planes, spots, tok, wl, wr, scale_hbm, cos_hbm, sin_hbm, cosq_hbm, sinq_hbm, kup, vup, q_hbm,
                k_out, v_out, flat_out, score_out, rot_out, turned_out,
                tokens, wlat, wrope, acc, acct, other, othert, spread, spreadt, xall, between, betweent,
                kbuf, vbuf, up, qbuf, blocked, wide, cos_ref, sin_ref, cosq, sinq, scale,
                tok_s, tok_r, own_s, zu_s, zd_s, z_r, x_s, x_r, y_s, y_r, d_s, d_r,
                acc_s, acc_r, g_s, g_r, j_s, f_s, f_r, m_s, m_r, p_s, p_r, up_s):
    s = lax.axis_index("sp")
    t = lax.axis_index("tp")
    z = t // CORES
    c = t % CORES
    near = spots == 4
    rows, lat = wl.shape
    rope = wr.shape[0]
    span = tok.shape[1]
    heads, kw = kup.shape[1:]
    vw = vup.shape[2]
    quarter = rows // 4
    eighth = quarter // 2
    rpart = rope // 4
    part = span // PARTS
    q = s % 4
    sx = s + 1 - 2 * (s % 2)
    sy = s + 2 - 4 * ((s // 2) % 2)
    sd = sx + sy - s
    qx = q + 1 - 2 * (q % 2)
    qy = q + 2 - 4 * (q // 2)
    qd = 3 - q
    has_up = z + 1 < planes
    has_down = z > 0

    def dev(si, zi, ci):
        return {"sp": si, "tp": zi * CORES + ci}

    here = dev(s, z, 1 - c)
    barrier = pltpu.get_barrier_semaphore()

    def greet(where):
        pl.semaphore_signal(barrier, inc=1, device_id=where, device_id_type=pl.DeviceIdType.MESH)

    @pl.when(has_up)
    def _():
        greet(dev(s, z + 1, c))

    @pl.when(has_down)
    def _():
        greet(dev(s, z - 1, c))

    if near:
        greet(dev(sx, z, c))
        greet(dev(sy, z, c))
    else:
        for i in range(1, spots):
            greet(dev(lax.rem(s + i, spots), z, c))
    greet(here)

    def remote(src, dst, ss, rs, where):
        return pltpu.make_async_remote_copy(
            src_ref=src, dst_ref=dst, send_sem=ss, recv_sem=rs,
            device_id=where, device_id_type=pl.DeviceIdType.MESH)

    def each(copies, what):
        for p in copies:
            getattr(p, what)()

    def own_tok(u):
        cols = pl.ds(pl.multiple_of((u * CORES + c) * rows, 128), rows)
        return pltpu.make_async_copy(tok.at[0, :, cols], tokens.at[0, u], own_s.at[u])

    def part_tok(u):
        cols = pl.ds(pl.multiple_of((u * CORES + 1 - c) * rows, 128), rows)
        return remote(tok.at[0, :, cols], tokens.at[1, u], tok_s.at[u], tok_r.at[u], here)

    own_w = [pltpu.make_async_copy(wl, wlat.at[z], own_s.at[planes]),
             pltpu.make_async_copy(wr, wrope.at[z], own_s.at[planes + 1])]
    each(own_w, "start")
    place = pl.ds(pl.multiple_of(s * span, 128), span)
    loads = [(kup, kbuf), (vup, vbuf), (cos_hbm.at[:, place], cos_ref), (sin_hbm.at[:, place], sin_ref),
             (cosq_hbm, cosq), (sinq_hbm, sinq), (scale_hbm, scale), (q_hbm, qbuf)]
    loads = [pltpu.make_async_copy(a, b, up_s.at[i]) for i, (a, b) in enumerate(loads)]
    each(loads, "start")
    for u in range(planes):
        own_tok(u).start()
    each(own_w, "wait")
    pl.semaphore_wait(barrier, (2 if near else spots - 1) + 1 + has_up.astype(jnp.int32) + has_down.astype(jnp.int32))

    def block(u, of, k, ss, rs, where):
        rng = pl.ds(pl.multiple_of(of * quarter + k * eighth, 16), eighth)
        out = [remote(wlat.at[u, rng], wlat.at[u, rng], ss(k), rs(k), where)]
        if k == 0:
            rng = pl.ds(pl.multiple_of(of * rpart, 16), rpart)
            out.append(remote(wrope.at[u, rng], wrope.at[u, rng], ss(2), rs(2), where))
        return out

    def extra(u):
        hops = jnp.where((u > z) | ((u == z) & ~has_up), u, planes - 1 - u)
        return jnp.where(hops == planes - 1, 2, 1)

    def extra_to(u, up_way):
        hops = planes - 1 - u if up_way else u
        return jnp.where(hops == planes - 1, 2, 1)

    def z_block(u, k, ss, where):
        if k < 2:
            return block(u, q, k, ss, lambda i: z_r.at[i, u], where)
        return block(u, qd, 3 - k, lambda i: ss(3 + i), lambda i: z_r.at[3 + i, u], where)

    def z_up(u, k):
        return z_block(u, k, lambda i: zu_s.at[i, u], dev(s, z + 1, c))

    def z_down(u, k):
        return z_block(u, k, lambda i: zd_s.at[i, u], dev(s, z - 1, c))

    def z_in(u, k):
        return z_block(u, k, lambda i: zu_s.at[i, u], here)

    def sent(u, k, up_way):
        return k < 3 or extra_to(u, up_way) == 2

    def by_y(u):
        return (u + c) % 2 == 0

    def piece(u, of, k, ss, rs, where):
        return block(u, of, k, lambda i: ss.at[i, u], lambda i: rs.at[i, u], where)

    def x_copy(u, k):
        return piece(u, q, k, x_s, x_r, dev(sx, z, c))

    def y_copy(u, k):
        return piece(u, q, k, y_s, y_r, dev(sy, z, c))

    def x_in(u, k):
        return piece(u, qx, k, x_s, x_r, here)

    def y_in(u, k):
        return piece(u, qy, k, y_s, y_r, here)

    def relay(u, of, where):
        return block(u, of, 0, lambda i: d_s.at[i // 2, u], lambda i: d_r.at[i // 2, u], where)

    def dy_copy(u):
        return relay(u, qx, dev(sy, z, c))

    def dx_copy(u):
        return relay(u, qy, dev(sx, z, c))

    def d_in(u):
        return relay(u, qd, here)

    for k in range(4):
        @pl.when(has_up & sent(z, k, True))
        def _():
            each(z_up(z, k), "start")

        @pl.when(has_down & sent(z, k, False))
        def _():
            each(z_down(z, k), "start")

    for u in range(planes):
        part_tok(u).start()
    each(loads, "wait")
    ks = kbuf[...].astype(F32)
    vs = vbuf[...].astype(F32)
    for h in range(heads):
        up[:, h * kw:(h + 1) * kw] = ks[:, h, :].astype(BF16)
        up[:, heads * kw + h * vw:heads * kw + (h + 1) * vw] = vs[:, h, :].astype(BF16)
    for b in range(CORES):
        query = qbuf[b].astype(F32)
        turned_out[b] = turn(query[:, kw:], cosq[...], sinq[...]).astype(BF16)
        tiled = jnp.concatenate([query[:, :kw]] * heads, axis=1)
        row = lax.broadcasted_iota(jnp.int32, tiled.shape, 0)
        col = lax.broadcasted_iota(jnp.int32, tiled.shape, 1)
        blocked[b] = jnp.where(col // kw == row, tiled, 0.0).astype(BF16)
    contract = (((1,), (1,)), ((), ()))

    def block_dot(u):
        x = tokens[:, u].reshape(CORES * span, rows)
        return (jnp.dot(x, wlat[u], preferred_element_type=F32),
                lax.dot_general(wrope[u], x, contract, preferred_element_type=F32))

    def valid(u):
        return (u >= 0) & (u < planes)

    def relayed(u):
        return (u != z) & (extra(u) == 1)

    def step(d, carry):
        for k in range(4):
            for sign in (-1, 1):
                u = z + sign * d

                @pl.when(valid(u) & sent(u, k, sign < 0))
                def _():
                    each(z_in(u, k), "wait_recv")
                    if sign < 0:
                        @pl.when(has_up)
                        def _():
                            each(z_up(u, k), "start")
                    else:
                        @pl.when(has_down)
                        def _():
                            each(z_down(u, k), "start")
                    if k < 2:
                        each(x_copy(u, k), "start")
                        each(y_copy(u, k), "start")
            if k == 0:
                for sign in (-1, 1):
                    u = z + sign * (d - 1)

                    @pl.when(valid(u) & (d > 1) & relayed(u))
                    def _():
                        @pl.when(by_y(u))
                        def _():
                            each(x_in(u, 0), "wait_recv")
                            each(dy_copy(u), "start")

                        @pl.when(~by_y(u))
                        def _():
                            each(y_in(u, 0), "wait_recv")
                            each(dx_copy(u), "start")
            if k == 1:
                @pl.when(d == 1)
                def _():
                    for u in range(planes):
                        own_tok(u).wait()
                        part_tok(u).wait()
                    a, b = block_dot(z)
                    acc[...] = a
                    acct[...] = b

                for sign in (-1, 1):
                    u = z + sign * (d - 2)

                    @pl.when(valid(u) & (d > 2))
                    def _():
                        @pl.when(~relayed(u) | ~by_y(u))
                        def _():
                            each(x_in(u, 0), "wait_recv")

                        @pl.when(~relayed(u) | by_y(u))
                        def _():
                            each(y_in(u, 0), "wait_recv")

                        each(x_in(u, 1), "wait_recv")
                        each(y_in(u, 1), "wait_recv")

                        @pl.when(relayed(u))
                        def _():
                            each(d_in(u), "wait_recv")
                        a, b = block_dot(u)
                        acc[...] += a
                        acct[...] += b
        return carry

    lax.fori_loop(1, planes + 2, step, 0)

    swaps = [remote(acc.at[pl.ds(span, span)], other, acc_s.at[0], acc_r.at[0], here),
             remote(acct.at[:, pl.ds(span, span)], othert, acc_s.at[1], acc_r.at[1], here)]
    each(swaps, "start")
    each(swaps, "wait")
    latent = acc[:span] + other[...]
    ropes = acct[:, :span] + othert[...]
    scaled = latent * lax.rsqrt(jnp.mean(latent * latent, axis=-1, keepdims=True) + 1e-06)
    spread[z] = (scaled * scale[...]).astype(BF16)
    swapped = jnp.concatenate([ropes[rope // 2:], ropes[:rope // 2]], axis=0)
    spreadt[z] = (ropes * cos_ref[...] + swapped * sin_ref[...]).astype(BF16)

    def cut(k):
        return pl.ds(pl.multiple_of(k * part, 16), part)

    def lanes(si):
        return pl.ds(pl.multiple_of(si * span, 128), span)

    def act(k, main, turned, what):
        getattr(main, what)()

        @pl.when(k == 0)
        def _():
            getattr(turned, what)()

    def g_copy(u, k, zi, slot, what):
        act(k, remote(spread.at[u, cut(k)], spread.at[u, cut(k)], g_s.at[slot, k, u], g_r.at[k, u], dev(s, zi, c)),
            remote(spreadt.at[u], spreadt.at[u], g_s.at[slot, PARTS, u], g_r.at[PARTS, u], dev(s, zi, c)), what)

    def f_copy(u, k, where, si, what):
        act(k, remote(spread.at[u, cut(k)], xall.at[c, si, cut(k)], f_s.at[k, u], f_r.at[k, si], where),
            remote(spreadt.at[u], rot_out.at[c, :, lanes(si)], f_s.at[PARTS, u], f_r.at[PARTS, si], where), what)

    def b_copy(u, k, what):
        where = dev(jnp.where(k < 2, sx, sy), z, c)
        act(k, remote(spread.at[u, cut(k)], between.at[cut(k)], f_s.at[k, u], m_r.at[k], where),
            remote(spreadt.at[u], betweent, f_s.at[PARTS, u], m_r.at[PARTS], where), what)

    def m_copy(k, what):
        si = jnp.where(k < 2, sx, sy)
        where = dev(jnp.where(k < 2, sy, sx), z, c)
        act(k, remote(between.at[cut(k)], xall.at[c, si, cut(k)], m_s.at[k], f_r.at[k, si], where),
            remote(betweent, rot_out.at[c, :, lanes(si)], m_s.at[PARTS], f_r.at[PARTS, si], where), what)

    def p_own(k, what):
        act(k, remote(spread.at[s, cut(k)], xall.at[c, s, cut(k)], p_s.at[k, s], p_r.at[k, s], here),
            remote(spreadt.at[s], rot_out.at[c, :, lanes(s)], p_s.at[PARTS, s], p_r.at[PARTS, s], here), what)

    def p_copy(ci, si, k, what):
        turned = rot_out.at[ci, :, lanes(si)]
        act(k, remote(xall.at[ci, si, cut(k)], xall.at[ci, si, cut(k)], p_s.at[k, si], p_r.at[k, si], here),
            remote(turned, turned, p_s.at[PARTS, si], p_r.at[PARTS, si], here), what)

    def deliver(u, k):
        if near:
            @pl.when((u != s) & (u != sd))
            def _():
                f_copy(u, k, dev(u, z, c), s, "start")

            @pl.when(u == sd)
            def _():
                b_copy(u, k, "start")
        else:
            @pl.when(u != s)
            def _():
                f_copy(u, k, dev(u, z, c), s, "start")

        @pl.when(u == s)
        def _():
            p_own(k, "start")

    def gone(u, what):
        def one(k, carry):
            @pl.when(u != s)
            def _():
                f_copy(u, k, here, s, what)

            @pl.when((u <= z) & ups(u))
            def _():
                g_copy(u, k, z, 0, what)

            @pl.when((u >= z) & downs(u))
            def _():
                g_copy(u, k, z, 1, what)
            return carry
        lax.fori_loop(0, PARTS, one, 0)

    jump = planes > 2
    across = jump & ((z == 0) | (z == planes - 1))
    end = planes - 1 - z

    def g_jump(k, what):
        act(k, remote(spread.at[z, cut(k)], spread.at[z, cut(k)], j_s.at[k], g_r.at[k, z], dev(s, end, c)),
            remote(spreadt.at[z], spreadt.at[z], j_s.at[PARTS], g_r.at[PARTS, z], dev(s, end, c)), what)

    if jump:
        @pl.when(across)
        def _():
            def far(k, carry):
                g_jump(k, "start")
                return carry

            lax.fori_loop(0, PARTS, far, 0)

    def first(k, carry):
        @pl.when(has_up)
        def _():
            g_copy(z, k, z + 1, 0, "start")

        @pl.when(has_down)
        def _():
            g_copy(z, k, z - 1, 1, "start")
        return carry

    lax.fori_loop(0, PARTS, first, 0)

    def second(k, carry):
        deliver(z, k)
        return carry

    lax.fori_loop(0, PARTS, second, 0)

    def drain(u, carry):
        for k in range(4):
            @pl.when((u >= z) & has_down & sent(u, k, False))
            def _():
                each(z_down(u, k), "wait_send")

            @pl.when((u <= z) & has_up & sent(u, k, True))
            def _():
                each(z_up(u, k), "wait_send")

        for k in range(2):
            @pl.when(u != z)
            def _():
                each(x_copy(u, k), "wait_send")
                each(y_copy(u, k), "wait_send")

        @pl.when(relayed(u))
        def _():
            each(dy_copy(u), "wait_send")
        return carry

    lax.fori_loop(0, planes, drain, 0)

    def fill(ci, si, x):
        keys = jnp.dot(x, up[:, :heads * kw], preferred_element_type=F32)
        values = jnp.dot(x, up[:, heads * kw:], preferred_element_type=F32)
        where = pl.ds(pl.multiple_of(si * span * heads, 128), span * heads)
        for h in range(heads):
            wide[0, pl.ds(h, span, stride=heads), :] = keys[:, h * kw:(h + 1) * kw]
        k_out[ci, where, :] = wide[0].astype(BF16)
        for h in range(heads):
            wide[1, pl.ds(h, span, stride=heads), :] = values[:, h * vw:(h + 1) * vw]
        v_out[ci, where, :] = wide[1].astype(BF16)
        flat_out[ci, lanes(si), :] = values.astype(BF16)
        score_out[ci, :, lanes(si)] = lax.dot_general(blocked[ci], keys.astype(BF16), contract, preferred_element_type=F32)

    inner = z < planes // 2
    edge = (z == 0) | (z == planes - 1)
    pace = jnp.where(edge, PARTS, 2 * PARTS)

    def ups(u):
        return has_up & ((u > 0) | (z + 1 < planes - 1) | (z == 0))

    def downs(u):
        return has_down & ((u < planes - 1) | (z > 1) | (z == planes - 1))

    def begin(u):
        far = jnp.where(u > z, u - z, z - u)
        side = jnp.where((u > z) == inner, 0, PARTS)
        return jnp.where(u == z, -LAG, pace * (far - 1) + side)

    last = max(PARTS * (planes - 2), 2 * PARTS * (planes - 3) + PARTS) + PARTS + LAG - 1

    def go(n, carry):
        for toward in (True, False):
            i = n if toward else n - PARTS
            d = lax.div(i, pace) + 1
            k = lax.rem(i, pace)
            up_way = ~inner if toward else inner
            u = jnp.where(up_way, z - d, z + d)

            @pl.when(valid(u) & (i >= 0) & (k < PARTS))
            def _():
                g_copy(u, k, z, 0, "wait_recv")

                @pl.when(up_way & ups(u))
                def _():
                    g_copy(u, k, z + 1, 0, "start")

                @pl.when(~up_way & downs(u))
                def _():
                    g_copy(u, k, z - 1, 1, "start")
                deliver(u, k)

        def arrive(k, si):
            f_copy(0, k, here, si, "wait_recv")
            p_copy(c, si, k, "start")

        k = n - begin(s) - LAG
        if near:
            @pl.when((k >= 0) & (k < PARTS))
            def _():
                arrive(k, sx)
                arrive(k, sy)

            kx = n - begin(sy) - LAG

            @pl.when((kx >= 0) & (kx < 2))
            def _():
                m_wait(kx)
                m_copy(kx, "start")

            ky = n - begin(sx) - LAG

            @pl.when((ky >= 2) & (ky < PARTS))
            def _():
                m_wait(ky)
                m_copy(ky, "start")

            kd = k - 3

            @pl.when((kd >= 0) & (kd < PARTS))
            def _():
                arrive(kd, sd)
        else:
            @pl.when((k >= 0) & (k < PARTS))
            def _():
                def other_spot(i, carry):
                    arrive(k, lax.rem(s + i, spots))
                    return carry
                lax.fori_loop(1, spots, other_spot, 0)

        i = n - last

        if near:
            i = jnp.where(n >= last + 4, n - last - 1, jnp.where(n == last + 3, spots, i))

        @pl.when((i >= 0) & (i < spots))
        def _():
            if near:
                si = jnp.where(i == 0, s, jnp.where(i == 1, sx, jnp.where(i == 2, sy, sd)))
            else:
                si = lax.rem(s + i, spots)

            @pl.when(i == 0)
            def _():
                rot_out[c, :, lanes(s)] = spreadt[s]
                xall[c, s] = spread[s]

            fill(c, si, xall[c, si])

            def landed(k, carry):
                p_copy(1 - c, si, k, "wait_recv")
                return carry

            lax.fori_loop(0, PARTS, landed, 0)
            fill(1 - c, si, xall[1 - c, si])
        return carry

    def m_wait(k):
        act(k, remote(between.at[cut(k)], between.at[cut(k)], m_s.at[k], m_r.at[k], here),
            remote(betweent, betweent, m_s.at[PARTS], m_r.at[PARTS], here), "wait_recv")

    lax.fori_loop(0, last + spots + (1 if near else 0), go, 0)

    def leave(u, carry):
        gone(u, "wait_send")

        def one(k, carry):
            p_copy(c, u, k, "wait_send")
            return carry

        lax.fori_loop(0, PARTS, one, 0)
        return carry

    lax.fori_loop(0, planes, leave, 0)

    def ended(k, carry):
        if near:
            m_copy(k, "wait_send")
        if jump:
            @pl.when(across)
            def _():
                g_jump(k, "wait_send")
        return carry

    lax.fori_loop(0, PARTS, ended, 0)


def read_kernel(k_ref, v_ref, flat_ref, score_ref, rot_ref, turned_ref, plain_hbm, value_hbm, rot_hbm, read_hbm, reads, sems):
    heads, length = score_ref.shape[1:]
    kw = k_ref.shape[2]
    vw = v_ref.shape[2]
    rope = rot_ref.shape[1]
    copies = [pltpu.make_async_copy(a, b, sems.at[i])
              for i, (a, b) in enumerate([(k_ref, plain_hbm), (v_ref, value_hbm), (rot_ref, rot_hbm)])]
    for copy in copies:
        copy.start()
    for b in range(CORES):
        scores = score_ref[b] + jnp.dot(turned_ref[b], rot_ref[b], preferred_element_type=F32)
        scores = scores * (1.0 / (kw + rope) ** 0.5)
        weights = jnp.exp(scores - jnp.max(scores, axis=-1, keepdims=True))
        total = jnp.sum(weights, axis=-1, keepdims=True)
        mixed = jnp.dot(weights.astype(BF16), flat_ref[b], preferred_element_type=F32) / total
        for h in range(heads):
            reads[b, h:h + 1, :] = mixed[h:h + 1, h * vw:(h + 1) * vw].astype(BF16)
    last = pltpu.make_async_copy(reads, read_hbm, sems.at[3])
    last.start()
    for copy in copies:
        copy.wait()
    last.wait()


def body(planes, spots, tokens, latent_down, rope_weight, norm_scale, key_up, value_up, query):
    span = tokens.shape[1]
    rows, lat = latent_down.shape
    rope = rope_weight.shape[1]
    heads, kw = key_up.shape[1:]
    vw = value_up.shape[2]
    length = spots * span
    cosine, sine = turn_tables(np.arange(length + 1), rope)
    vmem = pl.BlockSpec(memory_space=pltpu.VMEM)
    hbm = pl.BlockSpec(memory_space=pltpu.HBM)
    dma = pltpu.SemaphoreType.DMA
    operands = (tokens, latent_down, rope_weight.T, norm_scale.reshape(1, lat),
                jnp.asarray(np.ascontiguousarray(cosine[:length].T)), jnp.asarray(np.ascontiguousarray(sine[:length].T)),
                jnp.asarray(cosine[length:]), jnp.asarray(sine[length:]), key_up, value_up, query)
    results = pl.pallas_call(
        functools.partial(move_kernel, planes, spots),
        out_shape=(pltpu.VMEM((CORES, length * heads, kw), BF16),
                   pltpu.VMEM((CORES, length * heads, vw), BF16),
                   pltpu.VMEM((CORES, length, heads * vw), BF16),
                   pltpu.VMEM((CORES, heads, length), F32),
                   pltpu.VMEM((CORES, rope, length), BF16),
                   pltpu.VMEM((CORES, heads, rope), BF16)),
        in_specs=[hbm] * len(operands),
        out_specs=(vmem,) * 6,
        scratch_shapes=[
            pltpu.VMEM((CORES, planes, span, rows), BF16),
            pltpu.VMEM((planes, rows, lat), BF16),
            pltpu.VMEM((planes, rope, rows), BF16),
            pltpu.VMEM((CORES * span, lat), F32),
            pltpu.VMEM((rope, CORES * span), F32),
            pltpu.VMEM((span, lat), F32),
            pltpu.VMEM((rope, span), F32),
            pltpu.VMEM((planes, span, lat), BF16),
            pltpu.VMEM((planes, rope, span), BF16),
            pltpu.VMEM((CORES, spots, span, lat), BF16),
            pltpu.VMEM((span, lat), BF16),
            pltpu.VMEM((rope, span), BF16),
            pltpu.VMEM(key_up.shape, BF16),
            pltpu.VMEM(value_up.shape, BF16),
            pltpu.VMEM((lat, heads * (kw + vw)), BF16),
            pltpu.VMEM(query.shape, BF16),
            pltpu.VMEM((CORES, heads, heads * kw), BF16),
            pltpu.VMEM((2, span * heads, kw), F32),
            pltpu.VMEM((rope, span), F32),
            pltpu.VMEM((rope, span), F32),
            pltpu.VMEM((1, rope), F32),
            pltpu.VMEM((1, rope), F32),
            pltpu.VMEM((1, lat), F32),
            dma((planes,)), dma((planes,)), dma((planes + 2,)),
            dma((6, planes)), dma((6, planes)), dma((6, planes)),
            dma((3, planes)), dma((3, planes)), dma((3, planes)), dma((3, planes)),
            dma((2, planes)), dma((2, planes)),
            dma((2,)), dma((2,)),
            dma((2, PARTS + 1, planes)), dma((PARTS + 1, planes)), dma((PARTS + 1,)),
            dma((PARTS + 1, planes)), dma((PARTS + 1, spots)),
            dma((PARTS + 1,)), dma((PARTS + 1,)),
            dma((PARTS + 1, spots)), dma((PARTS + 1, spots)),
            dma((8,)),
        ],
        compiler_params=pltpu.CompilerParams(collective_id=0, has_side_effects=True, vmem_limit_bytes=VMEM_BYTES),
    )(*[pltpu.with_memory_space_constraint(v, pltpu.HBM) for v in operands])
    plain, value, rot, read = pl.pallas_call(
        read_kernel,
        out_shape=(jax.ShapeDtypeStruct((CORES, length * heads, kw), BF16),
                   jax.ShapeDtypeStruct((CORES, length * heads, vw), BF16),
                   jax.ShapeDtypeStruct((CORES, rope, length), BF16),
                   jax.ShapeDtypeStruct((CORES, heads, vw), BF16)),
        in_specs=[vmem] * 6,
        out_specs=(hbm,) * 4,
        scratch_shapes=[pltpu.VMEM((CORES, heads, vw), BF16), dma((4,))],
        compiler_params=pltpu.CompilerParams(vmem_limit_bytes=VMEM_BYTES // 2),
    )(*results)
    return (plain.reshape(CORES, length, heads, kw), value.reshape(CORES, length, heads, vw), jnp.swapaxes(rot, 1, 2), read)


def solution(mesh):
    planes = mesh.shape["tp"] // CORES
    spots = mesh.shape["sp"]
    assert planes == spots and spots % 4 == 0
    in_specs = (
        P("tp", "sp", None),
        P("tp", None),
        P("tp", None),
        P(),
        P(None, "tp", None),
        P(None, "tp", None),
        P("sp", "tp", None),
    )
    out_specs = (
        P("sp", None, "tp", None),
        P("sp", None, "tp", None),
        P("sp", None, None),
        P("sp", "tp", None),
    )
    return jax.shard_map(functools.partial(body, planes, spots), mesh=mesh, in_specs=in_specs,
                         out_specs=out_specs, check_vma=False)
```

```python
import functools

import numpy as np
import jax
import jax.numpy as jnp
from jax import lax
from jax.sharding import PartitionSpec as P
from jax.experimental import pallas as pl
from jax.experimental.pallas import tpu as pltpu

CORES = 2
PARTS = 4
LAG = 4
VMEM_BYTES = 32 * 1024 * 1024
BF16 = jnp.bfloat16
F32 = jnp.float32


def turn_tables(positions, width):
    half = width // 2
    freqs = (1.0 / np.float32(10000.0) ** (np.arange(half, dtype=np.float32) * np.float32(2.0) / np.float32(width))).astype(np.float32)
    angles = positions.astype(np.float32)[:, None] * freqs
    cosine = np.cos(angles).astype(np.float32)
    sine = np.sin(angles).astype(np.float32)
    return np.concatenate([cosine, cosine], -1), np.concatenate([-sine, sine], -1)


def turn(part, cosine, sine):
    half = part.shape[-1] // 2
    swapped = jnp.concatenate([part[:, half:], part[:, :half]], axis=-1)
    return part * cosine + swapped * sine


def move_kernel(planes, spots, tok, wl, wr, scale_hbm, cos_hbm, sin_hbm, cosq_hbm, sinq_hbm, kup, vup, q_hbm,
                k_out, v_out, flat_out, score_out, rot_out, turned_out,
                tokens, wlat, wrope, acc, acct, other, othert, spread, spreadt, xall, between, betweent,
                kbuf, vbuf, up, qbuf, blocked, wide, cos_ref, sin_ref, cosq, sinq, scale,
                tok_s, own_s, zu_s, zd_s, z_r, x_s, x_r, y_s, y_r, d_s, d_r,
                acc_s, acc_r, g_s, g_r, j_s, f_s, f_r, m_s, m_r, p_s, p_r, up_s):
    s = lax.axis_index("sp")
    t = lax.axis_index("tp")
    z = t // CORES
    c = t % CORES
    near = spots == 4
    rows, lat = wl.shape
    rope = wr.shape[0]
    span = tok.shape[1]
    heads, kw = kup.shape[1:]
    vw = vup.shape[2]
    quarter = rows // 4
    eighth = quarter // 2
    rpart = rope // 4
    part = span // PARTS
    q = s % 4
    sx = s + 1 - 2 * (s % 2)
    sy = s + 2 - 4 * ((s // 2) % 2)
    sd = sx + sy - s
    qx = q + 1 - 2 * (q % 2)
    qy = q + 2 - 4 * (q // 2)
    qd = 3 - q
    has_up = z + 1 < planes
    has_down = z > 0

    def dev(si, zi, ci):
        return {"sp": si, "tp": zi * CORES + ci}

    here = dev(s, z, 1 - c)
    barrier = pltpu.get_barrier_semaphore()

    def greet(where):
        pl.semaphore_signal(barrier, inc=1, device_id=where, device_id_type=pl.DeviceIdType.MESH)

    @pl.when(has_up)
    def _():
        greet(dev(s, z + 1, c))

    @pl.when(has_down)
    def _():
        greet(dev(s, z - 1, c))

    if near:
        greet(dev(sx, z, c))
        greet(dev(sy, z, c))
    else:
        for i in range(1, spots):
            greet(dev(lax.rem(s + i, spots), z, c))
    greet(here)

    def remote(src, dst, ss, rs, where):
        return pltpu.make_async_remote_copy(
            src_ref=src, dst_ref=dst, send_sem=ss, recv_sem=rs,
            device_id=where, device_id_type=pl.DeviceIdType.MESH)

    def each(copies, what):
        for p in copies:
            getattr(p, what)()

    def own_tok(u):
        cols = pl.ds(pl.multiple_of((u * CORES + c) * rows, 128), rows)
        return pltpu.make_async_copy(tok.at[0, :, cols], tokens.at[0, u], own_s.at[0])

    def part_tok(u):
        cols = pl.ds(pl.multiple_of((u * CORES + 1 - c) * rows, 128), rows)
        return remote(tok.at[0, :, cols], tokens.at[1, u], tok_s.at[0], tok_s.at[1], here)

    own_w = [pltpu.make_async_copy(wl, wlat.at[z], own_s.at[1]),
             pltpu.make_async_copy(wr, wrope.at[z], own_s.at[2])]
    each(own_w, "start")
    place = pl.ds(pl.multiple_of(s * span, 128), span)
    loads = [(kup, kbuf), (vup, vbuf), (cos_hbm.at[:, place], cos_ref), (sin_hbm.at[:, place], sin_ref),
             (cosq_hbm, cosq), (sinq_hbm, sinq), (scale_hbm, scale), (q_hbm, qbuf)]
    loads = [pltpu.make_async_copy(a, b, up_s.at[i]) for i, (a, b) in enumerate(loads)]
    each(loads, "start")
    for u in range(planes):
        own_tok(u).start()
    each(own_w, "wait")
    pl.semaphore_wait(barrier, (2 if near else spots - 1) + 1 + has_up.astype(jnp.int32) + has_down.astype(jnp.int32))

    def block(u, of, k, ss, rs, where):
        rng = pl.ds(pl.multiple_of(of * quarter + k * eighth, 16), eighth)
        out = [remote(wlat.at[u, rng], wlat.at[u, rng], ss(k), rs(k), where)]
        if k == 0:
            rng = pl.ds(pl.multiple_of(of * rpart, 16), rpart)
            out.append(remote(wrope.at[u, rng], wrope.at[u, rng], ss(2), rs(2), where))
        return out

    def extra(u):
        hops = jnp.where((u > z) | ((u == z) & ~has_up), u, planes - 1 - u)
        return jnp.where(hops == planes - 1, 2, 1)

    def extra_to(u, up_way):
        hops = planes - 1 - u if up_way else u
        return jnp.where(hops == planes - 1, 2, 1)

    def z_block(u, k, ss, where):
        if k < 2:
            return block(u, q, k, ss, lambda i: z_r.at[i, u], where)
        return block(u, qd, 3 - k, ss, lambda i: z_r.at[3 + i, u], where)

    def z_up(u, k):
        return z_block(u, k, lambda i: zu_s.at[i // 2, u], dev(s, z + 1, c))

    def z_down(u, k):
        return z_block(u, k, lambda i: zd_s.at[i // 2, u], dev(s, z - 1, c))

    def z_in(u, k):
        return z_block(u, k, lambda i: zu_s.at[i // 2, u], here)

    def sent(u, k, up_way):
        return k < 3 or extra_to(u, up_way) == 2

    def by_y(u):
        return (u + c) % 2 == 0

    def x_copy(u, k):
        return block(u, q, k, lambda i: x_s.at[i // 2], lambda i: x_r.at[i, u], dev(sx, z, c))

    def y_copy(u, k):
        return block(u, q, k, lambda i: y_s.at[i // 2], lambda i: y_r.at[i, u], dev(sy, z, c))

    def x_in(u, k):
        return block(u, qx, k, lambda i: x_s.at[i // 2], lambda i: x_r.at[i, u], here)

    def y_in(u, k):
        return block(u, qy, k, lambda i: y_s.at[i // 2], lambda i: y_r.at[i, u], here)

    def relay(u, of, where):
        return block(u, of, 0, lambda i: d_s.at[i // 2, u], lambda i: d_r.at[i // 2, u], where)

    def dy_copy(u):
        return relay(u, qx, dev(sy, z, c))

    def dx_copy(u):
        return relay(u, qy, dev(sx, z, c))

    def d_in(u):
        return relay(u, qd, here)

    for k in range(4):
        @pl.when(has_up & sent(z, k, True))
        def _():
            each(z_up(z, k), "start")

        @pl.when(has_down & sent(z, k, False))
        def _():
            each(z_down(z, k), "start")

    for u in range(planes):
        part_tok(u).start()
    each(loads, "wait")
    ks = kbuf[...].astype(F32)
    vs = vbuf[...].astype(F32)
    for h in range(heads):
        up[:, h * kw:(h + 1) * kw] = ks[:, h, :].astype(BF16)
        up[:, heads * kw + h * vw:heads * kw + (h + 1) * vw] = vs[:, h, :].astype(BF16)
    for b in range(CORES):
        query = qbuf[b].astype(F32)
        turned_out[b] = turn(query[:, kw:], cosq[...], sinq[...]).astype(BF16)
        tiled = jnp.concatenate([query[:, :kw]] * heads, axis=1)
        row = lax.broadcasted_iota(jnp.int32, tiled.shape, 0)
        col = lax.broadcasted_iota(jnp.int32, tiled.shape, 1)
        blocked[b] = jnp.where(col // kw == row, tiled, 0.0).astype(BF16)
    contract = (((1,), (1,)), ((), ()))

    def block_dot(u):
        x = tokens[:, u].reshape(CORES * span, rows)
        return (jnp.dot(x, wlat[u], preferred_element_type=F32),
                lax.dot_general(wrope[u], x, contract, preferred_element_type=F32))

    def valid(u):
        return (u >= 0) & (u < planes)

    def relayed(u):
        return (u != z) & (extra(u) == 1)

    def step(d, carry):
        for k in range(4):
            for sign in (-1, 1):
                u = z + sign * d

                @pl.when(valid(u) & sent(u, k, sign < 0))
                def _():
                    each(z_in(u, k), "wait_recv")
                    if sign < 0:
                        @pl.when(has_up)
                        def _():
                            each(z_up(u, k), "start")
                    else:
                        @pl.when(has_down)
                        def _():
                            each(z_down(u, k), "start")
                    if k < 2:
                        each(x_copy(u, k), "start")
                        each(y_copy(u, k), "start")
            if k == 0:
                for sign in (-1, 1):
                    u = z + sign * (d - 1)

                    @pl.when(valid(u) & (d > 1) & relayed(u))
                    def _():
                        @pl.when(by_y(u))
                        def _():
                            each(x_in(u, 0), "wait_recv")
                            each(dy_copy(u), "start")

                        @pl.when(~by_y(u))
                        def _():
                            each(y_in(u, 0), "wait_recv")
                            each(dx_copy(u), "start")
            if k == 1:
                @pl.when(d == 1)
                def _():
                    pltpu.make_async_copy(tokens.at[0], tokens.at[0], own_s.at[0]).wait()
                    remote(tokens.at[1], tokens.at[1], tok_s.at[0], tok_s.at[1], here).wait()
                    a, b = block_dot(z)
                    acc[...] = a
                    acct[...] = b

                for sign in (-1, 1):
                    u = z + sign * (d - 2)

                    @pl.when(valid(u) & (d > 2))
                    def _():
                        @pl.when(~relayed(u) | ~by_y(u))
                        def _():
                            each(x_in(u, 0), "wait_recv")

                        @pl.when(~relayed(u) | by_y(u))
                        def _():
                            each(y_in(u, 0), "wait_recv")

                        each(x_in(u, 1), "wait_recv")
                        each(y_in(u, 1), "wait_recv")

                        @pl.when(relayed(u))
                        def _():
                            each(d_in(u), "wait_recv")
                        a, b = block_dot(u)
                        acc[...] += a
                        acct[...] += b
        return carry

    lax.fori_loop(1, planes + 2, step, 0)

    swaps = [remote(acc.at[pl.ds(span, span)], other, acc_s.at[0], acc_r.at[0], here),
             remote(acct.at[:, pl.ds(span, span)], othert, acc_s.at[1], acc_r.at[1], here)]
    each(swaps, "start")
    each(swaps, "wait")
    latent = acc[:span] + other[...]
    ropes = acct[:, :span] + othert[...]
    scaled = latent * lax.rsqrt(jnp.mean(latent * latent, axis=-1, keepdims=True) + 1e-06)
    spread[z] = (scaled * scale[...]).astype(BF16)
    swapped = jnp.concatenate([ropes[rope // 2:], ropes[:rope // 2]], axis=0)
    spreadt[z] = (ropes * cos_ref[...] + swapped * sin_ref[...]).astype(BF16)

    def cut(k):
        return pl.ds(pl.multiple_of(k * part, 16), part)

    def lanes(si):
        return pl.ds(pl.multiple_of(si * span, 128), span)

    def act(k, main, turned, what):
        getattr(main, what)()

        @pl.when(k == 0)
        def _():
            getattr(turned, what)()

    def g_copy(u, k, zi, slot, what):
        act(k, remote(spread.at[u, cut(k)], spread.at[u, cut(k)], g_s.at[0, slot, u], g_r.at[k, u], dev(s, zi, c)),
            remote(spreadt.at[u], spreadt.at[u], g_s.at[1, slot, u], g_r.at[PARTS, u], dev(s, zi, c)), what)

    def f_copy(u, k, where, si, what):
        act(k, remote(spread.at[u, cut(k)], xall.at[c, si, cut(k)], f_s.at[0], f_r.at[k, si], where),
            remote(spreadt.at[u], rot_out.at[c, :, lanes(si)], f_s.at[1], f_r.at[PARTS, si], where), what)

    def b_copy(u, k, what):
        where = dev(jnp.where(k < 2, sx, sy), z, c)
        act(k, remote(spread.at[u, cut(k)], between.at[cut(k)], f_s.at[0], m_r.at[k], where),
            remote(spreadt.at[u], betweent, f_s.at[1], m_r.at[PARTS], where), what)

    def m_copy(k, what):
        si = jnp.where(k < 2, sx, sy)
        where = dev(jnp.where(k < 2, sy, sx), z, c)
        act(k, remote(between.at[cut(k)], xall.at[c, si, cut(k)], m_s.at[0], f_r.at[k, si], where),
            remote(betweent, rot_out.at[c, :, lanes(si)], m_s.at[1], f_r.at[PARTS, si], where), what)

    def p_own(k, what):
        act(k, remote(spread.at[s, cut(k)], xall.at[c, s, cut(k)], p_s.at[0], p_r.at[0, s], here),
            remote(spreadt.at[s], rot_out.at[c, :, lanes(s)], p_s.at[1], p_r.at[1, s], here), what)

    def p_copy(ci, si, k, what):
        turned = rot_out.at[ci, :, lanes(si)]
        act(k, remote(xall.at[ci, si, cut(k)], xall.at[ci, si, cut(k)], p_s.at[0], p_r.at[0, si], here),
            remote(turned, turned, p_s.at[1], p_r.at[1, si], here), what)

    def deliver(u, k):
        if near:
            @pl.when((u != s) & (u != sd))
            def _():
                f_copy(u, k, dev(u, z, c), s, "start")

            @pl.when(u == sd)
            def _():
                b_copy(u, k, "start")
        else:
            @pl.when(u != s)
            def _():
                f_copy(u, k, dev(u, z, c), s, "start")

        @pl.when(u == s)
        def _():
            p_own(k, "start")

    jump = planes > 2
    across = jump & ((z == 0) | (z == planes - 1))
    end = planes - 1 - z

    def g_jump(k, what):
        act(k, remote(spread.at[z, cut(k)], spread.at[z, cut(k)], j_s.at[0], g_r.at[k, z], dev(s, end, c)),
            remote(spreadt.at[z], spreadt.at[z], j_s.at[1], g_r.at[PARTS, z], dev(s, end, c)), what)

    if jump:
        @pl.when(across)
        def _():
            def far(k, carry):
                g_jump(k, "start")
                return carry

            lax.fori_loop(0, PARTS, far, 0)

    def first(k, carry):
        @pl.when(has_up)
        def _():
            g_copy(z, k, z + 1, 0, "start")

        @pl.when(has_down)
        def _():
            g_copy(z, k, z - 1, 1, "start")
        return carry

    lax.fori_loop(0, PARTS, first, 0)

    def second(k, carry):
        deliver(z, k)
        return carry

    lax.fori_loop(0, PARTS, second, 0)

    def left(ref, sem):
        remote(ref, ref, sem, sem, here).wait_send()

    def left_z(u, sems, up_way):
        for n in (1, 2):
            @pl.when(extra_to(u, up_way) == n)
            def _():
                left(wlat.at[u, pl.ds(0, (2 + n) * eighth)], sems.at[0, u])
                left(wrope.at[u, pl.ds(0, n * rpart)], sems.at[1, u])

    def drain(u, carry):
        @pl.when((u >= z) & has_down)
        def _():
            left_z(u, zd_s, False)

        @pl.when((u <= z) & has_up)
        def _():
            left_z(u, zu_s, True)

        @pl.when(relayed(u))
        def _():
            each(dy_copy(u), "wait_send")
        return carry

    lax.fori_loop(0, planes, drain, 0)
    for sems in (x_s, y_s):
        left(wlat.at[pl.ds(0, planes - 1), pl.ds(0, quarter)], sems.at[0])
        left(wrope.at[pl.ds(0, planes - 1), pl.ds(0, rpart)], sems.at[1])

    def fill(ci, si, x):
        keys = jnp.dot(x, up[:, :heads * kw], preferred_element_type=F32)
        values = jnp.dot(x, up[:, heads * kw:], preferred_element_type=F32)
        where = pl.ds(pl.multiple_of(si * span * heads, 128), span * heads)
        for h in range(heads):
            wide[0, pl.ds(h, span, stride=heads), :] = keys[:, h * kw:(h + 1) * kw]
        k_out[ci, where, :] = wide[0].astype(BF16)
        for h in range(heads):
            wide[1, pl.ds(h, span, stride=heads), :] = values[:, h * vw:(h + 1) * vw]
        v_out[ci, where, :] = wide[1].astype(BF16)
        flat_out[ci, lanes(si), :] = values.astype(BF16)
        score_out[ci, :, lanes(si)] = lax.dot_general(blocked[ci], keys.astype(BF16), contract, preferred_element_type=F32)

    inner = z < planes // 2
    edge = (z == 0) | (z == planes - 1)
    turns = 2 * PARTS
    rim_end = PARTS * max(planes - 3, 0)
    core_end = turns * (planes - 2) - PARTS

    def ups(u):
        return has_up & ((u > 0) | (z + 1 < planes - 1) | (z == 0))

    def downs(u):
        return has_down & ((u < planes - 1) | (z > 1) | (z == planes - 1))

    def begin(u):
        far = jnp.where(u > z, u - z, z - u)
        rim = jnp.where(far == planes - 1, rim_end, PARTS * (far - 1))
        near_side = jnp.where(far == 1, 0, turns * far - PARTS)
        core = jnp.where((u > z) == inner, near_side, turns * far)
        return jnp.where(u == z, 0, jnp.where(edge, rim, core))

    last = jnp.where(edge, rim_end, core_end) + PARTS + LAG - 1

    def go(n, carry):
        for toward in (False, True):
            up_way = ~inner if toward else inner
            if toward:
                rim = jnp.where(n < rim_end + PARTS, lax.div(n, PARTS) + 1, planes)
                core = jnp.where(n < PARTS, 1, lax.div(n + PARTS, turns))
                core = jnp.where((n >= PARTS) & (core < 2), planes, core)
            else:
                rim = jnp.where((n >= rim_end) & (n < rim_end + PARTS), planes - 1, planes)
                core = jnp.where(n < turns, planes, lax.div(n, turns))
            d = jnp.where(edge, rim, core)
            if not toward:
                up_way = jnp.where(edge, ~up_way, up_way)
            u = jnp.where(up_way, z - d, z + d)
            k = n - begin(u)

            @pl.when(valid(u) & (k >= 0) & (k < PARTS))
            def _():
                g_copy(u, k, z, 0, "wait_recv")

                @pl.when(up_way & ups(u))
                def _():
                    g_copy(u, k, z + 1, 0, "start")

                @pl.when(~up_way & downs(u))
                def _():
                    g_copy(u, k, z - 1, 1, "start")
                deliver(u, k)

        def arrive(k, si):
            f_copy(0, k, here, si, "wait_recv")
            p_copy(c, si, k, "start")

        k = n - begin(s) - LAG
        if near:
            @pl.when((k >= 0) & (k < PARTS))
            def _():
                arrive(k, sx)
                arrive(k, sy)

            kx = n - begin(sy) - LAG

            @pl.when((kx >= 0) & (kx < 2))
            def _():
                m_wait(kx)
                m_copy(kx, "start")

            ky = n - begin(sx) - LAG

            @pl.when((ky >= 2) & (ky < PARTS))
            def _():
                m_wait(ky)
                m_copy(ky, "start")

            kd = k - 3

            @pl.when((kd >= 0) & (kd < PARTS))
            def _():
                arrive(kd, sd)
        else:
            @pl.when((k >= 0) & (k < PARTS))
            def _():
                def other_spot(i, carry):
                    arrive(k, lax.rem(s + i, spots))
                    return carry
                lax.fori_loop(1, spots, other_spot, 0)

        if near:
            i = jnp.where(n == last - LAG, 0, jnp.where(n == last, 1, jnp.where(n > last + 2, n - last - 1, spots)))
        else:
            i = jnp.where(n == last - LAG, 0, jnp.where(n > last, n - last, spots))

        @pl.when((i >= 0) & (i < spots))
        def _():
            if near:
                si = jnp.where(i == 0, s, jnp.where(i == 1, sx, jnp.where(i == 2, sy, sd)))
            else:
                si = lax.rem(s + i, spots)

            @pl.when(i == 0)
            def _():
                rot_out[c, :, lanes(s)] = spreadt[s]
                xall[c, s] = spread[s]

            fill(c, si, xall[c, si])

            for ref, sem in ((xall.at[1 - c, si], p_r.at[0, si]), (rot_out.at[1 - c, :, lanes(si)], p_r.at[1, si])):
                remote(ref, ref, sem, sem, here).wait_recv()
            fill(1 - c, si, xall[1 - c, si])
        return carry

    def m_wait(k):
        act(k, remote(between.at[cut(k)], between.at[cut(k)], m_s.at[0], m_r.at[k], here),
            remote(betweent, betweent, m_s.at[1], m_r.at[PARTS], here), "wait_recv")

    lax.fori_loop(0, last + spots + (1 if near else 0), go, 0)

    def leave(u, carry):
        @pl.when((u <= z) & ups(u))
        def _():
            left(spread.at[u], g_s.at[0, 0, u])
            left(spreadt.at[u], g_s.at[1, 0, u])

        @pl.when((u >= z) & downs(u))
        def _():
            left(spread.at[u], g_s.at[0, 1, u])
            left(spreadt.at[u], g_s.at[1, 1, u])
        return carry

    lax.fori_loop(0, planes, leave, 0)
    left(spread.at[pl.ds(0, planes - 1)], f_s.at[0])
    left(spreadt.at[pl.ds(0, planes - 1)], f_s.at[1])
    left(xall.at[0], p_s.at[0])
    left(rot_out.at[0], p_s.at[1])
    if near:
        left(between, m_s.at[0])
        left(betweent, m_s.at[1])
    if jump:
        @pl.when(across)
        def _():
            left(spread.at[z], j_s.at[0])
            left(spreadt.at[z], j_s.at[1])


def read_kernel(k_ref, v_ref, flat_ref, score_ref, rot_ref, turned_ref, plain_hbm, value_hbm, rot_hbm, read_hbm, reads, sems):
    heads, length = score_ref.shape[1:]
    kw = k_ref.shape[2]
    vw = v_ref.shape[2]
    rope = rot_ref.shape[1]
    copies = [pltpu.make_async_copy(a, b, sems.at[i])
              for i, (a, b) in enumerate([(k_ref, plain_hbm), (v_ref, value_hbm), (rot_ref, rot_hbm)])]
    for copy in copies:
        copy.start()
    for b in range(CORES):
        scores = score_ref[b] + jnp.dot(turned_ref[b], rot_ref[b], preferred_element_type=F32)
        scores = scores * (1.0 / (kw + rope) ** 0.5)
        weights = jnp.exp(scores - jnp.max(scores, axis=-1, keepdims=True))
        total = jnp.sum(weights, axis=-1, keepdims=True)
        mixed = jnp.dot(weights.astype(BF16), flat_ref[b], preferred_element_type=F32) / total
        for h in range(heads):
            reads[b, h:h + 1, :] = mixed[h:h + 1, h * vw:(h + 1) * vw].astype(BF16)
    last = pltpu.make_async_copy(reads, read_hbm, sems.at[3])
    last.start()
    for copy in copies:
        copy.wait()
    last.wait()


def body(planes, spots, tokens, latent_down, rope_weight, norm_scale, key_up, value_up, query):
    span = tokens.shape[1]
    rows, lat = latent_down.shape
    rope = rope_weight.shape[1]
    heads, kw = key_up.shape[1:]
    vw = value_up.shape[2]
    length = spots * span
    cosine, sine = turn_tables(np.arange(length + 1), rope)
    vmem = pl.BlockSpec(memory_space=pltpu.VMEM)
    hbm = pl.BlockSpec(memory_space=pltpu.HBM)
    dma = pltpu.SemaphoreType.DMA
    operands = (tokens, latent_down, rope_weight.T, norm_scale.reshape(1, lat),
                jnp.asarray(np.ascontiguousarray(cosine[:length].T)), jnp.asarray(np.ascontiguousarray(sine[:length].T)),
                jnp.asarray(cosine[length:]), jnp.asarray(sine[length:]), key_up, value_up, query)
    results = pl.pallas_call(
        functools.partial(move_kernel, planes, spots),
        out_shape=(pltpu.VMEM((CORES, length * heads, kw), BF16),
                   pltpu.VMEM((CORES, length * heads, vw), BF16),
                   pltpu.VMEM((CORES, length, heads * vw), BF16),
                   pltpu.VMEM((CORES, heads, length), F32),
                   pltpu.VMEM((CORES, rope, length), BF16),
                   pltpu.VMEM((CORES, heads, rope), BF16)),
        in_specs=[hbm] * len(operands),
        out_specs=(vmem,) * 6,
        scratch_shapes=[
            pltpu.VMEM((CORES, planes, span, rows), BF16),
            pltpu.VMEM((planes, rows, lat), BF16),
            pltpu.VMEM((planes, rope, rows), BF16),
            pltpu.VMEM((CORES * span, lat), F32),
            pltpu.VMEM((rope, CORES * span), F32),
            pltpu.VMEM((span, lat), F32),
            pltpu.VMEM((rope, span), F32),
            pltpu.VMEM((planes, span, lat), BF16),
            pltpu.VMEM((planes, rope, span), BF16),
            pltpu.VMEM((CORES, spots, span, lat), BF16),
            pltpu.VMEM((span, lat), BF16),
            pltpu.VMEM((rope, span), BF16),
            pltpu.VMEM(key_up.shape, BF16),
            pltpu.VMEM(value_up.shape, BF16),
            pltpu.VMEM((lat, heads * (kw + vw)), BF16),
            pltpu.VMEM(query.shape, BF16),
            pltpu.VMEM((CORES, heads, heads * kw), BF16),
            pltpu.VMEM((2, span * heads, kw), F32),
            pltpu.VMEM((rope, span), F32),
            pltpu.VMEM((rope, span), F32),
            pltpu.VMEM((1, rope), F32),
            pltpu.VMEM((1, rope), F32),
            pltpu.VMEM((1, lat), F32),
            dma((2,)), dma((3,)),
            dma((2, planes)), dma((2, planes)), dma((6, planes)),
            dma((2,)), dma((3, planes)), dma((2,)), dma((3, planes)),
            dma((2, planes)), dma((2, planes)),
            dma((2,)), dma((2,)),
            dma((2, 2, planes)), dma((PARTS + 1, planes)), dma((2,)),
            dma((2,)), dma((PARTS + 1, spots)),
            dma((2,)), dma((PARTS + 1,)),
            dma((2,)), dma((2, spots)),
            dma((8,)),
        ],
        compiler_params=pltpu.CompilerParams(collective_id=0, has_side_effects=True, vmem_limit_bytes=VMEM_BYTES),
    )(*[pltpu.with_memory_space_constraint(v, pltpu.HBM) for v in operands])
    plain, value, rot, read = pl.pallas_call(
        read_kernel,
        out_shape=(jax.ShapeDtypeStruct((CORES, length * heads, kw), BF16),
                   jax.ShapeDtypeStruct((CORES, length * heads, vw), BF16),
                   jax.ShapeDtypeStruct((CORES, rope, length), BF16),
                   jax.ShapeDtypeStruct((CORES, heads, vw), BF16)),
        in_specs=[vmem] * 6,
        out_specs=(hbm,) * 4,
        scratch_shapes=[pltpu.VMEM((CORES, heads, vw), BF16), dma((4,))],
        compiler_params=pltpu.CompilerParams(vmem_limit_bytes=VMEM_BYTES // 2),
    )(*results)
    return (plain.reshape(CORES, length, heads, kw), value.reshape(CORES, length, heads, vw), jnp.swapaxes(rot, 1, 2), read)


def solution(mesh):
    planes = mesh.shape["tp"] // CORES
    spots = mesh.shape["sp"]
    assert planes == spots and spots % 4 == 0
    in_specs = (
        P("tp", "sp", None),
        P("tp", None),
        P("tp", None),
        P(),
        P(None, "tp", None),
        P(None, "tp", None),
        P("sp", "tp", None),
    )
    out_specs = (
        P("sp", None, "tp", None),
        P("sp", None, "tp", None),
        P("sp", None, None),
        P("sp", "tp", None),
    )
    return jax.shard_map(functools.partial(body, planes, spots), mesh=mesh, in_specs=in_specs,
                         out_specs=out_specs, check_vma=False)
```

```python
import functools

import numpy as np
import jax
import jax.numpy as jnp
from jax import lax
from jax.sharding import PartitionSpec as P
from jax.experimental import pallas as pl
from jax.experimental.pallas import tpu as pltpu

CORES = 2
PARTS = 4
LAG = 4
DLAG = 4
VMEM_BYTES = 32 * 1024 * 1024
BF16 = jnp.bfloat16
F32 = jnp.float32


def turn_tables(positions, width):
    half = width // 2
    freqs = (1.0 / np.float32(10000.0) ** (np.arange(half, dtype=np.float32) * np.float32(2.0) / np.float32(width))).astype(np.float32)
    angles = positions.astype(np.float32)[:, None] * freqs
    cosine = np.cos(angles).astype(np.float32)
    sine = np.sin(angles).astype(np.float32)
    return np.concatenate([cosine, cosine], -1), np.concatenate([-sine, sine], -1)


def turn(part, cosine, sine):
    half = part.shape[-1] // 2
    swapped = jnp.concatenate([part[:, half:], part[:, :half]], axis=-1)
    return part * cosine + swapped * sine


def move_kernel(planes, spots, tok, wl, wr, scale_hbm, cos_hbm, sin_hbm, cosq_hbm, sinq_hbm, kup, vup, q_hbm,
                k_out, v_out, flat_out, score_out, rot_out, turned_out,
                tokens, wlat, wrope, acc, acct, give, givet, other, othert, spread, spreadt, xall, between,
                kbuf, vbuf, up, qbuf, blocked, wide, cos_ref, sin_ref, cosq, sinq, scale,
                tok_s, own_s, zu_s, zd_s, z_r, xy_s, x_r, y_r, d_s, d_r,
                acc_s, acc_r, g_s, g_r, j_s, f_s, f_r, m_s, m_r, p_s, p_r, up_s):
    s = lax.axis_index("sp")
    t = lax.axis_index("tp")
    z = t // CORES
    c = t % CORES
    near = spots == 4
    rows, lat = wl.shape
    rope = wr.shape[0]
    span = tok.shape[1]
    heads, kw = kup.shape[1:]
    vw = vup.shape[2]
    quarter = rows // 4
    eighth = quarter // 2
    rpart = rope // 4
    part = span // PARTS
    q = s % 4
    sx = s + 1 - 2 * (s % 2)
    sy = s + 2 - 4 * ((s // 2) % 2)
    sd = sx + sy - s
    qx = q + 1 - 2 * (q % 2)
    qy = q + 2 - 4 * (q // 2)
    qd = 3 - q
    has_up = z + 1 < planes
    has_down = z > 0

    def dev(si, zi, ci):
        return {"sp": si, "tp": zi * CORES + ci}

    here = dev(s, z, 1 - c)
    barrier = pltpu.get_barrier_semaphore()

    def greet(where):
        pl.semaphore_signal(barrier, inc=1, device_id=where, device_id_type=pl.DeviceIdType.MESH)

    @pl.when(has_up)
    def _():
        greet(dev(s, z + 1, c))

    @pl.when(has_down)
    def _():
        greet(dev(s, z - 1, c))

    if near:
        greet(dev(sx, z, c))
        greet(dev(sy, z, c))
    else:
        for i in range(1, spots):
            greet(dev(lax.rem(s + i, spots), z, c))
    greet(here)

    def remote(src, dst, ss, rs, where):
        return pltpu.make_async_remote_copy(
            src_ref=src, dst_ref=dst, send_sem=ss, recv_sem=rs,
            device_id=where, device_id_type=pl.DeviceIdType.MESH)

    def each(copies, what):
        for p in copies:
            getattr(p, what)()

    def own_tok(u):
        cols = pl.ds(pl.multiple_of((u * CORES + c) * rows, 128), rows)
        return pltpu.make_async_copy(tok.at[0, :, cols], tokens.at[0, u], own_s.at[0])

    def part_tok(u):
        cols = pl.ds(pl.multiple_of((u * CORES + 1 - c) * rows, 128), rows)
        return remote(tok.at[0, :, cols], tokens.at[1, u], tok_s.at[0], tok_s.at[1], here)

    own_w = [pltpu.make_async_copy(wl, wlat.at[z], own_s.at[1]),
             pltpu.make_async_copy(wr, wrope.at[z], own_s.at[2])]
    each(own_w, "start")
    place = pl.ds(pl.multiple_of(s * span, 128), span)
    loads = [(kup, kbuf), (vup, vbuf), (cos_hbm.at[:, place], cos_ref), (sin_hbm.at[:, place], sin_ref),
             (cosq_hbm, cosq), (sinq_hbm, sinq), (scale_hbm, scale), (q_hbm, qbuf)]
    loads = [pltpu.make_async_copy(a, b, up_s.at[i]) for i, (a, b) in enumerate(loads)]
    each(loads, "start")
    for u in range(planes):
        own_tok(u).start()
    each(own_w, "wait")
    pl.semaphore_wait(barrier, (2 if near else spots - 1) + 1 + has_up.astype(jnp.int32) + has_down.astype(jnp.int32))

    def block(u, of, k, ss, rs, where):
        rng = pl.ds(pl.multiple_of(of * quarter + k * eighth, 16), eighth)
        out = [remote(wlat.at[u, rng], wlat.at[u, rng], ss, rs, where)]
        if k == 0:
            rng = pl.ds(pl.multiple_of(of * rpart, 16), rpart)
            out.append(remote(wrope.at[u, rng], wrope.at[u, rng], ss, rs, where))
        return out

    turn_rows = rope * span // lat
    middle = (span + turn_rows) // 2

    def got(sem, ref):
        remote(ref, ref, sem, sem, here).wait_recv()

    def left(ref, sem):
        remote(ref, ref, sem, sem, here).wait_send()

    wide_rows = eighth * lat // rows

    def sized(n):
        for a in range(1, CORES + 1):
            for b in range(1, planes + 1):
                if n % (a * b * 8) == 0 and n // (a * b) <= span:
                    return tokens.at[pl.ds(0, a), pl.ds(0, b), pl.ds(0, n // (a * b))]
        raise ValueError(n)

    def got_w(sem, k):
        got(sem, sized(wide_rows + (rpart if k in (0, 3) else 0)))

    def extra(u):
        hops = jnp.where((u > z) | ((u == z) & ~has_up), u, planes - 1 - u)
        return jnp.where(hops == planes - 1, 2, 1)

    def extra_to(u, up_way):
        hops = planes - 1 - u if up_way else u
        return jnp.where(hops == planes - 1, 2, 1)

    def z_block(u, k, ss, where):
        if k < 2:
            return block(u, q, k, ss.at[u], z_r.at[k, u], where)
        return block(u, qd, 3 - k, ss.at[u], z_r.at[k, u], where)

    def z_up(u, k):
        return z_block(u, k, zu_s, dev(s, z + 1, c))

    def z_down(u, k):
        return z_block(u, k, zd_s, dev(s, z - 1, c))

    def sent(u, k, up_way):
        return k < 3 or extra_to(u, up_way) == 2

    def by_y(u):
        return (u + c) % 2 == 0

    def x_copy(u, k):
        return block(u, q, k, xy_s.at[0], x_r.at[k, u], dev(sx, z, c))

    def y_copy(u, k):
        return block(u, q, k, xy_s.at[1], y_r.at[k, u], dev(sy, z, c))

    def dy_copy(u):
        return block(u, qx, 0, d_s.at[u], d_r.at[u], dev(sy, z, c))

    def dx_copy(u):
        return block(u, qy, 0, d_s.at[u], d_r.at[u], dev(sx, z, c))

    for k in range(4):
        @pl.when(has_up & sent(z, k, True))
        def _():
            each(z_up(z, k), "start")

        @pl.when(has_down & sent(z, k, False))
        def _():
            each(z_down(z, k), "start")

    for u in range(planes):
        part_tok(u).start()
    each(loads, "wait")
    ks = kbuf[...].astype(F32)
    vs = vbuf[...].astype(F32)
    for h in range(heads):
        up[:, h * kw:(h + 1) * kw] = ks[:, h, :].astype(BF16)
        up[:, heads * kw + h * vw:heads * kw + (h + 1) * vw] = vs[:, h, :].astype(BF16)
    for b in range(CORES):
        query = qbuf[b].astype(F32)
        turned_out[b] = turn(query[:, kw:], cosq[...], sinq[...]).astype(BF16)
        tiled = jnp.concatenate([query[:, :kw]] * heads, axis=1)
        row = lax.broadcasted_iota(jnp.int32, tiled.shape, 0)
        col = lax.broadcasted_iota(jnp.int32, tiled.shape, 1)
        blocked[b] = jnp.where(col // kw == row, tiled, 0.0).astype(BF16)
    contract = (((1,), (1,)), ((), ()))

    def block_dot(u):
        x = tokens[:, u].reshape(CORES * span, rows)
        return (jnp.dot(x, wlat[u], preferred_element_type=F32),
                lax.dot_general(wrope[u], x, contract, preferred_element_type=F32))

    def valid(u):
        return (u >= 0) & (u < planes)

    def relayed(u):
        return (u != z) & (extra(u) == 1)

    def add(u):
        @pl.when(~relayed(u) | ~by_y(u))
        def _():
            got_w(x_r.at[0, u], 0)

        @pl.when(~relayed(u) | by_y(u))
        def _():
            got_w(y_r.at[0, u], 0)

        got_w(x_r.at[1, u], 1)
        got_w(y_r.at[1, u], 1)

        @pl.when(relayed(u))
        def _():
            got_w(d_r.at[u], 0)
        a, b = block_dot(u)
        acc[...] += a
        acct[...] += b

    def step(d, carry):
        for sign in (-1, 1):
            u = z + sign * (d - 1)

            @pl.when(valid(u) & (d > 1) & relayed(u))
            def _():
                @pl.when(by_y(u))
                def _():
                    got_w(x_r.at[0, u], 0)
                    each(dy_copy(u), "start")

                @pl.when(~by_y(u))
                def _():
                    got_w(y_r.at[0, u], 0)
                    each(dx_copy(u), "start")
        for k in range(4):
            for sign in (-1, 1):
                u = z + sign * d

                @pl.when(valid(u) & sent(u, k, sign < 0))
                def _():
                    got_w(z_r.at[k, u], k)
                    if sign < 0:
                        @pl.when(has_up)
                        def _():
                            each(z_up(u, k), "start")
                    else:
                        @pl.when(has_down)
                        def _():
                            each(z_down(u, k), "start")
                    if k < 2:
                        each(x_copy(u, k), "start")
                        each(y_copy(u, k), "start")
            if k == 1:
                @pl.when(d == 1)
                def _():
                    pltpu.make_async_copy(tokens.at[0], tokens.at[0], own_s.at[0]).wait()
                    remote(tokens.at[1], tokens.at[1], tok_s.at[0], tok_s.at[1], here).wait()
                    a, b = block_dot(z)
                    acc[...] = a
                    acct[...] = b

                for sign in (-1, 1):
                    u = z + sign * (d - 2)

                    @pl.when(valid(u) & (d > 2))
                    def _():
                        add(u)
        return carry

    lax.fori_loop(1, planes + 1, step, 0)

    @pl.when((z == 0) | (z == planes - 1))
    def _():
        add(planes - 1 - z)

    give[...] = acc[span:].astype(BF16)
    givet[...] = acct[:, span:].astype(BF16)
    swaps = [remote(give, other, acc_s.at[0], acc_r.at[0], here),
             remote(givet, othert, acc_s.at[1], acc_r.at[1], here)]
    each(swaps, "start")
    each(swaps, "wait")
    latent = acc[:span] + other[...].astype(F32)
    ropes = acct[:, :span] + othert[...].astype(F32)
    scaled = latent * lax.rsqrt(jnp.mean(latent * latent, axis=-1, keepdims=True) + 1e-06)
    spread[z] = (scaled * scale[...]).astype(BF16)
    swapped = jnp.concatenate([ropes[rope // 2:], ropes[:rope // 2]], axis=0)
    spreadt[z] = (ropes * cos_ref[...] + swapped * sin_ref[...]).astype(BF16)

    def cut(k):
        return pl.ds(pl.multiple_of(k * part, 16), part)

    def lanes(si):
        return pl.ds(pl.multiple_of(si * span, 128), span)

    def act(k, main, turned, what):
        getattr(main, what)()

        @pl.when(k == 0)
        def _():
            getattr(turned, what)()

    def got_part(sem, k):
        @pl.when(k == 0)
        def _():
            got(sem, spread.at[0, pl.ds(0, part + turn_rows)])

        @pl.when(k > 0)
        def _():
            got(sem, spread.at[0, pl.ds(0, part)])

    def g_copy(u, k, zi, slot, what):
        act(k, remote(spread.at[u, cut(k)], spread.at[u, cut(k)], g_s.at[slot, u], g_r.at[k, u], dev(s, zi, c)),
            remote(spreadt.at[u], spreadt.at[u], g_s.at[slot, u], g_r.at[k, u], dev(s, zi, c)), what)

    def f_copy(u, k, where, si, what):
        act(k, remote(spread.at[u, cut(k)], xall.at[c, si, cut(k)], f_s.at[0], f_r.at[k, si], where),
            remote(spreadt.at[u], rot_out.at[c, :, lanes(si)], f_s.at[0], f_r.at[k, si], where), what)

    def p_own(k, what):
        act(k, remote(spread.at[s, cut(k)], xall.at[c, s, cut(k)], p_s.at[0], p_r.at[s], here),
            remote(spreadt.at[s], rot_out.at[c, :, lanes(s)], p_s.at[0], p_r.at[s], here), what)

    def p_copy(ci, si, k, what):
        turned = rot_out.at[ci, :, lanes(si)]
        act(k, remote(xall.at[ci, si, cut(k)], xall.at[ci, si, cut(k)], p_s.at[0], p_r.at[si], here),
            remote(turned, turned, p_s.at[0], p_r.at[si], here), what)

    def b_copy(u, k, what):
        remotely = remote(spread.at[u, cut(k)], between.at[cut(k - PARTS // 2)], f_s.at[0], m_r.at[k - PARTS // 2], dev(sy, z, c))
        getattr(remotely, what)()

    def m_copy(k):
        return remote(between.at[cut(k - PARTS // 2)], xall.at[c, sy, cut(k)], m_s.at[0], f_r.at[k, sy], dev(sx, z, c))

    def deliver(u, k):
        round_y = (u == sd) & (k >= PARTS // 2) if near else False

        @pl.when((u != s) & ~round_y if near else u != s)
        def _():
            f_copy(u, k, dev(u, z, c), s, "start")

        if near:
            @pl.when(round_y)
            def _():
                b_copy(u, k, "start")

        @pl.when(u == s)
        def _():
            p_own(k, "start")

    jump = planes > 2
    across = jump & ((z == 0) | (z == planes - 1))
    end = planes - 1 - z

    def g_jump(k, what):
        act(k, remote(spread.at[z, cut(k)], spread.at[z, cut(k)], j_s.at[0], g_r.at[k, z], dev(s, end, c)),
            remote(spreadt.at[z], spreadt.at[z], j_s.at[0], g_r.at[k, z], dev(s, end, c)), what)

    def first(k, carry):
        @pl.when(has_up)
        def _():
            g_copy(z, k, z + 1, 0, "start")

        @pl.when(has_down)
        def _():
            g_copy(z, k, z - 1, 1, "start")

        if jump:
            @pl.when(across)
            def _():
                g_jump(k, "start")
        return carry

    lax.fori_loop(0, PARTS, first, 0)

    def second(k, carry):
        deliver(z, k)
        return carry

    lax.fori_loop(0, PARTS, second, 0)

    def left_z(u, sems, up_way):
        for n in (1, 2):
            @pl.when(extra_to(u, up_way) == n)
            def _():
                left(sized((2 + n) * wide_rows + n * rpart), sems.at[u])

    def drain(u, carry):
        @pl.when((u >= z) & has_down)
        def _():
            left_z(u, zd_s, False)

        @pl.when((u <= z) & has_up)
        def _():
            left_z(u, zu_s, True)

        @pl.when(relayed(u))
        def _():
            left(sized(wide_rows + rpart), d_s.at[u])
        return carry

    lax.fori_loop(0, planes, drain, 0)
    for i in range(2):
        left(sized((planes - 1) * (2 * wide_rows + rpart)), xy_s.at[i])

    def fill(ci, si, x):
        keys = jnp.dot(x, up[:, :heads * kw], preferred_element_type=F32)
        values = jnp.dot(x, up[:, heads * kw:], preferred_element_type=F32)
        where = pl.ds(pl.multiple_of(si * span * heads, 128), span * heads)
        for h in range(heads):
            wide[0, pl.ds(h, span, stride=heads), :] = keys[:, h * kw:(h + 1) * kw]
        k_out[ci, where, :] = wide[0].astype(BF16)
        for h in range(heads):
            wide[1, pl.ds(h, span, stride=heads), :] = values[:, h * vw:(h + 1) * vw]
        v_out[ci, where, :] = wide[1].astype(BF16)
        flat_out[ci, lanes(si), :] = values.astype(BF16)
        score_out[ci, :, lanes(si)] = lax.dot_general(blocked[ci], keys.astype(BF16), contract, preferred_element_type=F32)

    inner = z < planes // 2
    edge = (z == 0) | (z == planes - 1)
    turns = 2 * PARTS
    rim_end = PARTS * max(planes - 3, 0)
    core_end = turns * (planes - 2) - PARTS

    def ups(u):
        return has_up & ((u > 0) | (z + 1 < planes - 1) | (z == 0))

    def downs(u):
        return has_down & ((u < planes - 1) | (z > 1) | (z == planes - 1))

    def begin(u):
        far = jnp.where(u > z, u - z, z - u)
        rim = jnp.where(far == planes - 1, rim_end, PARTS * (far - 1))
        near_side = jnp.where(far == 1, 0, turns * far - PARTS)
        core = jnp.where((u > z) == inner, near_side, turns * far)
        return jnp.where(u == z, 0, jnp.where(edge, rim, core))

    last = jnp.where(edge, rim_end, core_end) + PARTS + LAG - 1

    def go(n, carry):
        for toward in (False, True):
            up_way = ~inner if toward else inner
            if toward:
                rim = jnp.where(n < rim_end + PARTS, lax.div(n, PARTS) + 1, planes)
                core = jnp.where(n < PARTS, 1, lax.div(n + PARTS, turns))
                core = jnp.where((n >= PARTS) & (core < 2), planes, core)
            else:
                rim = jnp.where((n >= rim_end) & (n < rim_end + PARTS), planes - 1, planes)
                core = jnp.where(n < turns, planes, lax.div(n, turns))
            d = jnp.where(edge, rim, core)
            if not toward:
                up_way = jnp.where(edge, ~up_way, up_way)
            u = jnp.where(up_way, z - d, z + d)
            k = n - begin(u)

            @pl.when(valid(u) & (k >= 0) & (k < PARTS))
            def _():
                got_part(g_r.at[k, u], k)

                @pl.when(up_way & ups(u))
                def _():
                    g_copy(u, k, z + 1, 0, "start")

                @pl.when(~up_way & downs(u))
                def _():
                    g_copy(u, k, z - 1, 1, "start")
                deliver(u, k)

        def arrive(k, si):
            got_part(f_r.at[k, si], k)
            p_copy(c, si, k, "start")

        k = n - begin(s) - LAG

        @pl.when((k >= 0) & (k < PARTS))
        def _():
            if near:
                arrive(k, sx)
                arrive(k, sy)
            else:
                def other_spot(i, carry):
                    arrive(k, lax.rem(s + i, spots))
                    return carry
                lax.fori_loop(1, spots, other_spot, 0)

        if near:
            ky = n - begin(sx) - LAG

            @pl.when((ky >= PARTS // 2) & (ky < PARTS))
            def _():
                m_in = between.at[cut(ky - PARTS // 2)]
                remote(m_in, m_in, m_s.at[0], m_r.at[ky - PARTS // 2], here).wait_recv()
                m_copy(ky).start()

            kd = k - jnp.where(k <= PARTS // 2, 1, DLAG)

            @pl.when((kd >= 0) & (kd < PARTS) & ((k <= PARTS // 2) | (kd >= PARTS // 2)))
            def _():
                arrive(kd, sd)

        i = jnp.where(n < last, n - last + LAG, n - last + 2)
        i = jnp.where((n >= last - LAG + 2) & (n < last), -1, i)

        @pl.when(i >= 0)
        def _():
            if near:
                si = jnp.where(i < 2, s, jnp.where(i > 5, sd, jnp.where(lax.rem(i, 2) == 0, sx, sy)))
                mine = (i == 0) | (i == 2) | (i == 3) | (i == 6)
            else:
                si = lax.rem(s + lax.div(i, 2), spots)
                mine = lax.rem(i, 2) == 0

            @pl.when(i == 0)
            def _():
                rot_out[c, :, lanes(s)] = spreadt[s]
                xall[c, s] = spread[s]

            @pl.when(~mine)
            def _():
                got(p_r.at[si], spread.at[pl.ds(0, 2), pl.ds(0, middle)])

            ci = jnp.where(mine, c, 1 - c)
            fill(ci, si, xall[ci, si])
        return carry

    lax.fori_loop(0, last + 2 * spots - 2, go, 0)

    whole = spread.at[pl.ds(0, 2), pl.ds(0, middle)]

    def leave(u, carry):
        @pl.when((u <= z) & ups(u))
        def _():
            left(whole, g_s.at[0, u])

        @pl.when((u >= z) & downs(u))
        def _():
            left(whole, g_s.at[1, u])
        return carry

    lax.fori_loop(0, planes, leave, 0)
    left(xall.at[pl.ds(0, 2), pl.ds(0, planes - 1), pl.ds(0, middle)], f_s.at[0])
    left(xall.at[pl.ds(0, 2), pl.ds(0, spots), pl.ds(0, middle)], p_s.at[0])
    if near:
        left(between, m_s.at[0])
    if jump:
        @pl.when(across)
        def _():
            left(whole, j_s.at[0])


def read_kernel(k_ref, v_ref, flat_ref, score_ref, rot_ref, turned_ref, plain_hbm, value_hbm, rot_hbm, read_hbm, reads, sems):
    heads, length = score_ref.shape[1:]
    kw = k_ref.shape[2]
    vw = v_ref.shape[2]
    rope = rot_ref.shape[1]
    copies = [pltpu.make_async_copy(a, b, sems.at[i])
              for i, (a, b) in enumerate([(k_ref, plain_hbm), (v_ref, value_hbm), (rot_ref, rot_hbm)])]
    for copy in copies:
        copy.start()
    for b in range(CORES):
        scores = score_ref[b] + jnp.dot(turned_ref[b], rot_ref[b], preferred_element_type=F32)
        scores = scores * (1.0 / (kw + rope) ** 0.5)
        weights = jnp.exp(scores - jnp.max(scores, axis=-1, keepdims=True))
        total = jnp.sum(weights, axis=-1, keepdims=True)
        mixed = jnp.dot(weights.astype(BF16), flat_ref[b], preferred_element_type=F32) / total
        for h in range(heads):
            reads[b, h:h + 1, :] = mixed[h:h + 1, h * vw:(h + 1) * vw].astype(BF16)
    last = pltpu.make_async_copy(reads, read_hbm, sems.at[3])
    last.start()
    for copy in copies:
        copy.wait()
    last.wait()


def body(planes, spots, tokens, latent_down, rope_weight, norm_scale, key_up, value_up, query):
    span = tokens.shape[1]
    rows, lat = latent_down.shape
    rope = rope_weight.shape[1]
    heads, kw = key_up.shape[1:]
    vw = value_up.shape[2]
    length = spots * span
    cosine, sine = turn_tables(np.arange(length + 1), rope)
    vmem = pl.BlockSpec(memory_space=pltpu.VMEM)
    hbm = pl.BlockSpec(memory_space=pltpu.HBM)
    dma = pltpu.SemaphoreType.DMA
    operands = (tokens, latent_down, rope_weight.T, norm_scale.reshape(1, lat),
                jnp.asarray(np.ascontiguousarray(cosine[:length].T)), jnp.asarray(np.ascontiguousarray(sine[:length].T)),
                jnp.asarray(cosine[length:]), jnp.asarray(sine[length:]), key_up, value_up, query)
    results = pl.pallas_call(
        functools.partial(move_kernel, planes, spots),
        out_shape=(pltpu.VMEM((CORES, length * heads, kw), BF16),
                   pltpu.VMEM((CORES, length * heads, vw), BF16),
                   pltpu.VMEM((CORES, length, heads * vw), BF16),
                   pltpu.VMEM((CORES, heads, length), F32),
                   pltpu.VMEM((CORES, rope, length), BF16),
                   pltpu.VMEM((CORES, heads, rope), BF16)),
        in_specs=[hbm] * len(operands),
        out_specs=(vmem,) * 6,
        scratch_shapes=[
            pltpu.VMEM((CORES, planes, span, rows), BF16),
            pltpu.VMEM((planes, rows, lat), BF16),
            pltpu.VMEM((planes, rope, rows), BF16),
            pltpu.VMEM((CORES * span, lat), F32),
            pltpu.VMEM((rope, CORES * span), F32),
            pltpu.VMEM((span, lat), BF16),
            pltpu.VMEM((rope, span), BF16),
            pltpu.VMEM((span, lat), BF16),
            pltpu.VMEM((rope, span), BF16),
            pltpu.VMEM((planes, span, lat), BF16),
            pltpu.VMEM((planes, rope, span), BF16),
            pltpu.VMEM((CORES, spots, span, lat), BF16),
            pltpu.VMEM((span // 2, lat), BF16),
            pltpu.VMEM(key_up.shape, BF16),
            pltpu.VMEM(value_up.shape, BF16),
            pltpu.VMEM((lat, heads * (kw + vw)), BF16),
            pltpu.VMEM(query.shape, BF16),
            pltpu.VMEM((CORES, heads, heads * kw), BF16),
            pltpu.VMEM((2, span * heads, kw), F32),
            pltpu.VMEM((rope, span), F32),
            pltpu.VMEM((rope, span), F32),
            pltpu.VMEM((1, rope), F32),
            pltpu.VMEM((1, rope), F32),
            pltpu.VMEM((1, lat), F32),
            dma((2,)), dma((3,)),
            dma((planes,)), dma((planes,)), dma((4, planes)),
            dma((2,)), dma((2, planes)), dma((2, planes)),
            dma((planes,)), dma((planes,)),
            dma((2,)), dma((2,)),
            dma((2, planes)), dma((PARTS, planes)), dma((1,)),
            dma((1,)), dma((PARTS, spots)),
            dma((1,)), dma((PARTS // 2,)),
            dma((1,)), dma((spots,)),
            dma((8,)),
        ],
        compiler_params=pltpu.CompilerParams(collective_id=0, has_side_effects=True, vmem_limit_bytes=VMEM_BYTES),
    )(*[pltpu.with_memory_space_constraint(v, pltpu.HBM) for v in operands])
    plain, value, rot, read = pl.pallas_call(
        read_kernel,
        out_shape=(jax.ShapeDtypeStruct((CORES, length * heads, kw), BF16),
                   jax.ShapeDtypeStruct((CORES, length * heads, vw), BF16),
                   jax.ShapeDtypeStruct((CORES, rope, length), BF16),
                   jax.ShapeDtypeStruct((CORES, heads, vw), BF16)),
        in_specs=[vmem] * 6,
        out_specs=(hbm,) * 4,
        scratch_shapes=[pltpu.VMEM((CORES, heads, vw), BF16), dma((4,))],
        compiler_params=pltpu.CompilerParams(vmem_limit_bytes=VMEM_BYTES // 2),
    )(*results)
    return (plain.reshape(CORES, length, heads, kw), value.reshape(CORES, length, heads, vw), jnp.swapaxes(rot, 1, 2), read)


def solution(mesh):
    planes = mesh.shape["tp"] // CORES
    spots = mesh.shape["sp"]
    assert planes == spots and spots % 4 == 0
    in_specs = (
        P("tp", "sp", None),
        P("tp", None),
        P("tp", None),
        P(),
        P(None, "tp", None),
        P(None, "tp", None),
        P("sp", "tp", None),
    )
    out_specs = (
        P("sp", None, "tp", None),
        P("sp", None, "tp", None),
        P("sp", None, None),
        P("sp", "tp", None),
    )
    return jax.shard_map(functools.partial(body, planes, spots), mesh=mesh, in_specs=in_specs,
                         out_specs=out_specs, check_vma=False)
```
